32 devices in a mesh: grp: 2 (over y), sp: 4 (over z), tp: 4 (over x, core).
Axes of the slice: x: 2, y: 2, z: 4, core: 2. Of those that a mesh axis runs over, the one named last changes fastest.
Arguments:
- stream_in: bfloat16 [4096, 2048], P(('grp', 'sp')), parts along dimension 0, may hold values from -6 to 6
- query_wide: bfloat16 [4096, 1024], P(('grp', 'sp'), 'tp'), parts along dimension 0, may hold values from -6 to 6
- key_wide: bfloat16 [4096, 1024], P(('grp', 'sp'), 'tp'), parts along dimension 0, may hold values from -6 to 6
- value_wide: bfloat16 [4096, 2048], P(('grp', 'sp'), 'tp'), parts along dimension 0, may hold values from -6 to 6
- query_narrow: bfloat16 [4096, 512], P(('grp', 'sp'), 'tp'), parts along dimension 0, may hold values from -6 to 6
- key_narrow: bfloat16 [4096, 512], P(('grp', 'sp'), 'tp'), parts along dimension 0, may hold values from -6 to 6
- value_narrow: bfloat16 [4096, 1024], P(('grp', 'sp'), 'tp'), parts along dimension 0, may hold values from -6 to 6
- decay_wide: float32 [4, 4096], P('tp', ('grp', 'sp')), parts along dimension 1, may hold values from -1 to 0
- decay_narrow: float32 [4, 4096], P('tp', ('grp', 'sp')), parts along dimension 1, may hold values from -1 to 0
- gain_wide: float32 [2048], P('tp'), may hold values from 0.1 to 1.9
- gain_narrow: float32 [1024], P('tp'), may hold values from 0.1 to 1.9
- out_wide: bfloat16 [2048, 2048], P('tp'), may hold values from -0.109375 to 0.109375
- out_narrow: bfloat16 [1024, 2048], P('tp'), may hold values from -0.109375 to 0.109375
- mlp_gain: float32 [2048], replicated, may hold values from 0.1 to 1.9
- up_weight: bfloat16 [2048, 8192], P('sp', 'tp'), may hold values from -0.125 to 0.125
- down_weight: bfloat16 [8192, 2048], P('tp', 'sp'), may hold values from -0.0625 to 0.0625
Outputs:
- stream_out: bfloat16 [4096, 2048], P(('grp', 'sp', 'tp')), parts along dimension 0
The draws below stay inside these ranges and needn't reach their ends.
There are 2 independent parts, one for each index of `grp`. The reference program is written for one: setup_inputs(seed, part) draws one part's arguments, and reference() takes and returns one part's arrays. A program takes and returns all parts, laid end to end along the dimension named above; an argument that names none is the same for every part. Nothing has to cross between parts.
All inputs are finite; a program needn't handle non-finite values.
Results may differ from the reference program's by a relative error of at most 0.019.
Values may be sent and summed in bfloat16 or wider, within the bound.
A program may use at most 128 MiB of HBM per device.

```python
import math
import jax
import jax.numpy as jnp
from jax import lax

D = 2048
FF = 8192
HW = 4
HN = 4
DKW = 256
DVW = 512
DKN = 128
DVN = 256
TOK_DEV = 512
SEQUENCE_LENGTH = 2048
N_TP = 4


def decay_table(key, total_heads):
    shard_total = jax.random.split(key, 6)
    slow = jax.random.permutation(shard_total[0], total_heads) < total_heads // 2
    fast_rate = jnp.exp(jax.random.uniform(shard_total[1], (total_heads, 1), jnp.float32, math.log(1.0 / 50.0), math.log(1.0 / 30.0)))
    slow_rate = 0.4 / SEQUENCE_LENGTH
    block_factor = jnp.exp(jax.random.uniform(shard_total[2], (1, SEQUENCE_LENGTH // TOK_DEV), jnp.float32, math.log(0.5), math.log(2.0)))
    block_factor = jnp.repeat(block_factor, TOK_DEV, axis=1)
    roughness = jax.random.uniform(shard_total[3], (total_heads, SEQUENCE_LENGTH), jnp.float32, 0.5, 1.5)
    decay_rate = jnp.where(slow[:, None], slow_rate * block_factor, fast_rate * jnp.ones((1, SEQUENCE_LENGTH), jnp.float32))
    decay_rate = decay_rate * roughness
    segment_offset = jax.random.randint(shard_total[4], (total_heads, 2), 0, SEQUENCE_LENGTH)
    segment_length = jax.random.uniform(shard_total[5], (total_heads, 2), jnp.float32, math.log(0.5), math.log(0.8))
    token_position = jnp.arange(SEQUENCE_LENGTH, dtype=jnp.int32)
    segment_count = jnp.sum(jnp.where(token_position[None, None, :] == segment_offset[:, :, None], segment_length[:, :, None], 0.0), axis=1)
    return (segment_count - decay_rate).astype(jnp.float32)


def draw_decay_wide(key, part):
    return decay_table(jax.random.fold_in(key, 11), HW)


def draw_decay_narrow(key, part):
    return decay_table(jax.random.fold_in(key, 23), HN)


def block_scale(key, dims, shards, low, top_value):
    gain = 1.0
    for position, shards_of in shards:
        heights = jax.random.uniform(jax.random.fold_in(jax.random.fold_in(key, 6), position), (shards_of,), jnp.float32, low / len(shards), top_value / len(shards))
        gain = gain * jnp.repeat(jnp.exp(heights), dims[position] // shards_of).reshape((-1,) + (1,) * (len(dims) - 1 - position))
    return gain


def centred(key, dims, width, most, shards=(), kind=jnp.bfloat16):
    drawn = jax.random.normal(key, dims, jnp.float32) * width
    if len(shards) > 0:
        drawn = block_scale(key, dims, shards, -0.22, 0.18) * drawn
    return jnp.clip(drawn, min=-most, max=most).astype(kind)


def setup_inputs(seed: int = 0, part: int = 0) -> dict:
    splits = jax.random.split(jax.random.key(seed), 17)
    part_splits = jax.random.split(jax.random.fold_in(splits[16], part), 17)
    stream_in = centred(part_splits[0], (SEQUENCE_LENGTH, D), 1.0, 6.0, ((0, 4),))
    query_wide = centred(part_splits[1], (SEQUENCE_LENGTH, HW * DKW), 1.0, 6.0, ((0, 4), (1, 4)))
    key_wide = centred(part_splits[2], (SEQUENCE_LENGTH, HW * DKW), 1.0, 6.0, ((0, 4), (1, 4)))
    value_wide = centred(part_splits[3], (SEQUENCE_LENGTH, HW * DVW), 1.0, 6.0, ((0, 4), (1, 4)))
    query_narrow = centred(part_splits[4], (SEQUENCE_LENGTH, HN * DKN), 1.0, 6.0, ((0, 4), (1, 4)))
    key_narrow = centred(part_splits[5], (SEQUENCE_LENGTH, HN * DKN), 1.0, 6.0, ((0, 4), (1, 4)))
    value_narrow = centred(part_splits[6], (SEQUENCE_LENGTH, HN * DVN), 1.0, 6.0, ((0, 4), (1, 4)))
    decay_wide = draw_decay_wide(jax.random.fold_in(jax.random.fold_in(splits[16], part), 71), part)
    decay_narrow = draw_decay_narrow(jax.random.fold_in(jax.random.fold_in(splits[16], part), 71), part)
    gain_wide = jnp.clip(1.0 + 0.18 * jax.random.normal(splits[9], (HW * DVW,), jnp.float32), 0.1, 1.9)
    gain_narrow = jnp.clip(1.0 + 0.18 * jax.random.normal(splits[10], (HN * DVN,), jnp.float32), 0.1, 1.9)
    out_wide = centred(splits[11], (HW * DVW, D), (HW * DVW + HN * DVN) ** -0.5, 0.109375, ((0, 4),))
    out_narrow = centred(splits[12], (HN * DVN, D), (HW * DVW + HN * DVN) ** -0.5, 0.109375, ((0, 4),))
    mlp_gain = jnp.clip(1.0 + 0.18 * jax.random.normal(splits[13], (D,), jnp.float32), 0.1, 1.9)
    up_weight = centred(splits[14], (D, FF), D ** -0.5, 0.125, ((0, 4), (1, 4)))
    down_weight = centred(splits[15], (FF, D), FF ** -0.5, 0.0625, ((0, 4), (1, 4)))
    return dict(stream_in=stream_in, query_wide=query_wide, key_wide=key_wide, value_wide=value_wide, query_narrow=query_narrow, key_narrow=key_narrow, value_narrow=value_narrow, decay_wide=decay_wide, decay_narrow=decay_narrow, gain_wide=gain_wide, gain_narrow=gain_narrow, out_wide=out_wide, out_narrow=out_narrow, mlp_gain=mlp_gain, up_weight=up_weight, down_weight=down_weight)


EPS = 1e-06

def retain_group(queries, key_rows, value_rows, log_decay):
    total_heads = log_decay.shape[0]
    length = queries.shape[0]
    key_width = queries.shape[1] // total_heads
    value_width = value_rows.shape[1] // total_heads
    block_count = length // TOK_DEV
    query_blocks = queries.reshape(block_count, TOK_DEV, total_heads, key_width)
    key_blocks = key_rows.reshape(block_count, TOK_DEV, total_heads, key_width)
    value_blocks = value_rows.reshape(block_count, TOK_DEV, total_heads, value_width)
    decay_blocks = log_decay.reshape(total_heads, block_count, TOK_DEV).transpose(1, 0, 2)
    row_index = lax.broadcasted_iota(jnp.int32, (TOK_DEV, TOK_DEV), 0)
    col_index = lax.broadcasted_iota(jnp.int32, (TOK_DEV, TOK_DEV), 1)
    causal = (row_index >= col_index)[None]

    def advance(state, inputs):
        query_here, key_here, value_here, decay_here = inputs
        cumulative = jnp.cumsum(decay_here, axis=1)
        log_gap = cumulative[:, :, None] - cumulative[:, None, :]
        fading = jnp.where(causal, jnp.exp(jnp.where(causal, log_gap, 0.0)), 0.0)
        scores = jnp.einsum('ihd,jhd->hij', query_here.astype(jnp.float32), key_here.astype(jnp.float32))
        weights_low = lax.optimization_barrier((scores * key_width ** (-0.5) * fading).astype(jnp.bfloat16))
        within = jnp.einsum('hij,jhe->ihe', weights_low.astype(jnp.float32), value_here.astype(jnp.float32))
        carried = jnp.einsum('ihd,hde->ihe', query_here.astype(jnp.float32), state, precision=lax.Precision.HIGHEST) * jnp.exp(cumulative).T[:, :, None]
        to_end = jnp.exp(cumulative[:, -1:] - cumulative)
        keyed = lax.optimization_barrier((key_here.astype(jnp.float32) * key_width ** (-0.5) * to_end.T[:, :, None]).astype(jnp.bfloat16))
        local_state = jnp.einsum('jhd,jhe->hde', keyed.astype(jnp.float32), value_here.astype(jnp.float32))
        updated = jnp.exp(cumulative[:, -1])[:, None, None] * state + local_state
        return (updated, within + carried)
    start_state = jnp.zeros((total_heads, key_width, value_width), jnp.float32)
    _, retained = lax.scan(advance, start_state, (query_blocks, key_blocks, value_blocks, decay_blocks))
    return retained.reshape(length, total_heads, value_width)

def head_norm(retained, gain_values):
    centered = retained - lax.optimization_barrier(jnp.mean(retained, axis=-1, keepdims=True))
    scaled = centered * lax.rsqrt(lax.optimization_barrier(jnp.mean(centered * centered, axis=-1, keepdims=True)) + EPS)
    return (scaled.reshape(retained.shape[0], -1) * gain_values).astype(jnp.bfloat16)

def normalize(rows, gain_values):
    values = rows.astype(jnp.float32)
    scaled = values * lax.rsqrt(lax.optimization_barrier(jnp.mean(values * values, axis=-1, keepdims=True)) + EPS)
    return (scaled * gain_values).astype(jnp.bfloat16)

def reference(stream_in, query_wide, key_wide, value_wide, query_narrow, key_narrow, value_narrow, decay_wide, decay_narrow, gain_wide, gain_narrow, out_wide, out_narrow, mlp_gain, up_weight, down_weight):
    normed_wide = head_norm(retain_group(query_wide, key_wide, value_wide, decay_wide), gain_wide)
    normed_narrow = head_norm(retain_group(query_narrow, key_narrow, value_narrow, decay_narrow), gain_narrow)
    wide_cols = normed_wide.shape[1] // N_TP
    narrow_cols = normed_narrow.shape[1] // N_TP
    mix = jnp.zeros(stream_in.shape, jnp.float32)
    for member in range(N_TP):
        partial_sum = jnp.dot(normed_wide[:, member * wide_cols:(member + 1) * wide_cols], out_wide[member * wide_cols:(member + 1) * wide_cols], preferred_element_type=jnp.float32)
        partial_sum = partial_sum + jnp.dot(normed_narrow[:, member * narrow_cols:(member + 1) * narrow_cols], out_narrow[member * narrow_cols:(member + 1) * narrow_cols], preferred_element_type=jnp.float32)
        mix = mix + partial_sum.astype(jnp.bfloat16).astype(jnp.float32)
    middle = (stream_in.astype(jnp.float32) + mix).astype(jnp.bfloat16)
    normed_rows = normalize(middle, mlp_gain)
    hidden = jax.nn.relu(jnp.dot(normed_rows, up_weight, preferred_element_type=jnp.float32))
    hidden = (hidden * hidden).astype(jnp.bfloat16)
    unit_cols = hidden.shape[1] // N_TP
    channel = jnp.zeros(stream_in.shape, jnp.float32)
    for member in range(N_TP):
        partial_sum = jnp.dot(hidden[:, member * unit_cols:(member + 1) * unit_cols], down_weight[member * unit_cols:(member + 1) * unit_cols], preferred_element_type=jnp.float32)
        channel = channel + partial_sum.astype(jnp.bfloat16).astype(jnp.float32)
    return (middle.astype(jnp.float32) + channel).astype(jnp.bfloat16)
```

```python
import jax
import jax.numpy as jnp
from jax import lax
from jax.sharding import PartitionSpec as P

EPS = 1e-06


def shifted(x, axis, step):
    size = lax.axis_size(axis)
    pairs = [(i, i + step) for i in range(size) if 0 <= i + step < size]
    return lax.ppermute(x, axis, pairs)


def incoming_state(states, log_factors, axis):
    size, mine = lax.axis_size(axis), lax.axis_index(axis)
    received = [
        [shifted(part.astype(jnp.bfloat16), axis, k) for part in states] for k in range(1, size)
    ]
    logs = [lax.all_gather(part, axis) for part in log_factors]
    index = jnp.arange(size)
    totals = [jnp.zeros(part.shape, jnp.float32) for part in states]
    for k in range(1, size):
        between = ((index > mine - k) & (index < mine))[:, None]
        for i, log in enumerate(logs):
            fade = jnp.exp(jnp.sum(jnp.where(between, log, 0.0), axis=0))
            fade = jnp.where(mine >= k, fade, 0.0)
            totals[i] = totals[i] + fade[:, None, None] * received[k - 1][i].astype(jnp.float32)
    return totals


def own_part(weight, dim, part, parts):
    width = weight.shape[dim] // parts
    return lax.dynamic_slice_in_dim(weight, part * width, width, dim)


def swap_parts(x, reach):
    groups, size = lax.axis_size("grp"), lax.axis_size("sp")
    return [
        lax.ppermute(
            x,
            ("grp", "sp"),
            [(((g + k) % groups) * size + i, g * size + i) for g in range(groups) for i in reach],
        )
        for k in range(1, groups)
    ]


def weight_chunks(weight, dim):
    groups, size = lax.axis_size("grp"), lax.axis_size("sp")
    group, mine = lax.axis_index("grp"), lax.axis_index("sp")
    chunks = [
        [own_part(weight, dim, (group + k) % groups, groups) for k in range(groups)]
    ]
    from_left, from_right = {}, {}
    left = right = chunks[0][0]
    for step in range(1, size):
        left = lax.ppermute(left, "sp", [(i, i + 1) for i in range(step - 1, size - 1)])
        right = lax.ppermute(right, "sp", [(i, i - 1) for i in range(1, size - step + 1)])
        from_left[step] = [left] + swap_parts(left, range(step, size))
        from_right[step] = [right] + swap_parts(right, range(size - step))
    for j in range(1, size):
        chunks.append(
            [
                jnp.where(mine + j < size, after, before)
                for after, before in zip(from_right[j], from_left[size - j])
            ]
        )
    return chunks


def scatter_sum(x):
    size, member = lax.axis_size("tp"), lax.axis_index("tp")
    if size & (size - 1):
        return lax.psum_scatter(x, "tp", scatter_dimension=0, tiled=True).astype(jnp.float32)
    rest, width = size, x.shape[1]
    portion = x.shape[0] // size
    bit = 1
    total = x
    while bit < size:
        rest //= 2
        here = (member // bit) % 2
        split = total.reshape(rest, 2, portion, width)
        keep = lax.dynamic_index_in_dim(split, here, 1, keepdims=False)
        send = lax.dynamic_index_in_dim(split, 1 - here, 1, keepdims=False).astype(jnp.bfloat16)
        got = lax.ppermute(send, "tp", [(i, i ^ bit) for i in range(size)])
        total = keep.astype(jnp.float32) + got.astype(jnp.float32)
        bit *= 2
    return total.reshape(portion, width)


def gather_rows(x):
    size, member = lax.axis_size("tp"), lax.axis_index("tp")
    if size & (size - 1):
        return lax.all_gather(x, "tp", axis=0, tiled=True)
    portion, width = x.shape
    whole = x[None]
    bit = size // 2
    while bit:
        here = (member // bit) % 2
        got = lax.ppermute(whole, "tp", [(i, i ^ bit) for i in range(size)])
        first = jnp.where(here == 0, whole, got)
        second = jnp.where(here == 0, got, whole)
        whole = jnp.stack([first, second], axis=1).reshape(-1, portion, width)
        bit //= 2
    return whole.reshape(size * portion, width)


def retain_local(queries, key_rows, value_rows, log_decay):
    total_heads = log_decay.shape[0]
    length = queries.shape[0]
    key_width = queries.shape[1] // total_heads
    value_width = value_rows.shape[1] // total_heads
    query_heads = queries.reshape(length, total_heads, key_width)
    key_heads = key_rows.reshape(length, total_heads, key_width)
    value_heads = value_rows.reshape(length, total_heads, value_width)
    cumulative = jnp.cumsum(log_decay, axis=1)
    row_index = lax.broadcasted_iota(jnp.int32, (length, length), 0)
    col_index = lax.broadcasted_iota(jnp.int32, (length, length), 1)
    causal = (row_index >= col_index)[None]
    log_gap = cumulative[:, :, None] - cumulative[:, None, :]
    fading = jnp.where(causal, jnp.exp(jnp.where(causal, log_gap, 0.0)), 0.0)
    scores = jnp.einsum("ihd,jhd->hij", query_heads, key_heads, preferred_element_type=jnp.float32)
    weights_low = (scores * key_width ** (-0.5) * fading).astype(jnp.bfloat16)
    within = jnp.einsum(
        "hij,jhe->ihe", weights_low, value_heads, preferred_element_type=jnp.float32
    )
    to_end = jnp.exp(cumulative[:, -1:] - cumulative)
    keyed = (key_heads.astype(jnp.float32) * key_width ** (-0.5) * to_end.T[:, :, None]).astype(
        jnp.bfloat16
    )
    local_state = jnp.einsum("jhd,jhe->hde", keyed, value_heads, preferred_element_type=jnp.float32)
    return (query_heads, cumulative, within, cumulative[:, -1], local_state)


def finish(query_heads, cumulative, within, incoming, gain_values):
    carried = (
        jnp.einsum(
            "ihd,hde->ihe",
            query_heads,
            incoming.astype(jnp.bfloat16),
            preferred_element_type=jnp.float32,
        )
        * jnp.exp(cumulative).T[:, :, None]
    )
    retained = within + carried
    centered = retained - jnp.mean(retained, axis=-1, keepdims=True)
    scaled = centered * lax.rsqrt(jnp.mean(centered * centered, axis=-1, keepdims=True) + EPS)
    return (scaled.reshape(retained.shape[0], -1) * gain_values).astype(jnp.bfloat16)


def normalize(rows, gain_values):
    values = rows.astype(jnp.float32)
    scaled = values * lax.rsqrt(jnp.mean(values * values, axis=-1, keepdims=True) + EPS)
    return (scaled * gain_values).astype(jnp.bfloat16)


def on_device(
    stream_in,
    query_wide,
    key_wide,
    value_wide,
    query_narrow,
    key_narrow,
    value_narrow,
    decay_wide,
    decay_narrow,
    gain_wide,
    gain_narrow,
    out_wide,
    out_narrow,
    mlp_gain,
    up_weight,
    down_weight,
):
    length = stream_in.shape[0]
    portion = length // lax.axis_size("tp")
    member = lax.axis_index("tp")
    up_chunks = weight_chunks(up_weight, 0)
    down_chunks = weight_chunks(down_weight, 1)
    wide_query, wide_cum, wide_within, wide_log, wide_state = retain_local(
        query_wide, key_wide, value_wide, decay_wide
    )
    thin_query, thin_cum, thin_within, thin_log, thin_state = retain_local(
        query_narrow, key_narrow, value_narrow, decay_narrow
    )
    wide_incoming, thin_incoming = incoming_state(
        (wide_state, thin_state), (wide_log, thin_log), "sp"
    )
    normed_wide = finish(wide_query, wide_cum, wide_within, wide_incoming, gain_wide)
    normed_thin = finish(thin_query, thin_cum, thin_within, thin_incoming, gain_narrow)
    mixed = scatter_sum(
        (
            jnp.dot(normed_wide, out_wide, preferred_element_type=jnp.float32)
            + jnp.dot(normed_thin, out_narrow, preferred_element_type=jnp.float32)
        ).astype(jnp.bfloat16)
    )
    stream_rows = lax.dynamic_slice_in_dim(stream_in, member * portion, portion, 0)
    middle = (stream_rows.astype(jnp.float32) + mixed).astype(jnp.bfloat16)
    normed = gather_rows(normalize(middle, mlp_gain))
    groups, size = lax.axis_size("grp"), lax.axis_size("sp")
    group, mine = lax.axis_index("grp"), lax.axis_index("sp")
    depth = up_weight.shape[0]
    turned = jnp.roll(normed, -mine * depth, axis=1)
    turned = turned.reshape(length, size, groups, depth // groups)
    turned = jnp.roll(turned, -group, axis=2).reshape(length, -1)
    up_full = jnp.concatenate([part for chunk in up_chunks for part in chunk], axis=0)
    raised = jax.nn.relu(jnp.dot(turned, up_full, preferred_element_type=jnp.float32))
    hidden = (raised * raised).astype(jnp.bfloat16)
    blocks = []
    for chunk in down_chunks:
        partial = jnp.concatenate(
            [jnp.dot(hidden, part, preferred_element_type=jnp.float32) for part in chunk], axis=1
        )
        blocks.append(scatter_sum(partial.astype(jnp.bfloat16)))
    channel = jnp.stack(blocks, axis=1).reshape(portion, size, groups, -1)
    channel = jnp.roll(channel, group, axis=2).reshape(portion, -1)
    channel = jnp.roll(channel, mine * down_weight.shape[1], axis=1)
    return (middle.astype(jnp.float32) + channel).astype(jnp.bfloat16)


def solution(mesh):
    placed = (
        P(("grp", "sp"), None),
        P(("grp", "sp"), "tp"),
        P(("grp", "sp"), "tp"),
        P(("grp", "sp"), "tp"),
        P(("grp", "sp"), "tp"),
        P(("grp", "sp"), "tp"),
        P(("grp", "sp"), "tp"),
        P("tp", ("grp", "sp")),
        P("tp", ("grp", "sp")),
        P("tp"),
        P("tp"),
        P("tp", None),
        P("tp", None),
        P(),
        P("sp", "tp"),
        P("tp", "sp"),
    )
    return jax.shard_map(
        on_device,
        mesh=mesh,
        in_specs=placed,
        out_specs=P(("grp", "sp", "tp"), None),
        check_vma=False,
    )
```

```python
import jax
import jax.numpy as jnp
from jax import lax
from jax.sharding import PartitionSpec as P

EPS = 1e-06


def shifted(x, axis, step):
    size = lax.axis_size(axis)
    pairs = [(i, i + step) for i in range(size) if 0 <= i + step < size]
    return lax.ppermute(x, axis, pairs)


def incoming_state(states, log_factors, axis):
    size, mine = lax.axis_size(axis), lax.axis_index(axis)
    received = [
        [shifted(part.astype(jnp.bfloat16), axis, k) for part in states] for k in range(1, size)
    ]
    logs = [lax.all_gather(part, axis) for part in log_factors]
    index = jnp.arange(size)
    totals = [jnp.zeros(part.shape, jnp.float32) for part in states]
    for k in range(1, size):
        between = ((index > mine - k) & (index < mine))[:, None]
        for i, log in enumerate(logs):
            fade = jnp.exp(jnp.sum(jnp.where(between, log, 0.0), axis=0))
            fade = jnp.where(mine >= k, fade, 0.0)
            totals[i] = totals[i] + fade[:, None, None] * received[k - 1][i].astype(jnp.float32)
    return totals


def own_part(weight, dim, part, parts):
    width = weight.shape[dim] // parts
    return lax.dynamic_slice_in_dim(weight, part * width, width, dim)


def swap_parts(x, reach):
    groups, size = lax.axis_size("grp"), lax.axis_size("sp")
    return [
        lax.ppermute(
            x,
            ("grp", "sp"),
            [(((g + k) % groups) * size + i, g * size + i) for g in range(groups) for i in reach],
        )
        for k in range(1, groups)
    ]


def weight_chunks(weight, dim):
    groups, size = lax.axis_size("grp"), lax.axis_size("sp")
    group, mine = lax.axis_index("grp"), lax.axis_index("sp")
    chunks = [
        [own_part(weight, dim, (group + k) % groups, groups) for k in range(groups)]
    ]
    from_left, from_right = {}, {}
    left = right = chunks[0][0]
    for step in range(1, size):
        left = lax.ppermute(left, "sp", [(i, i + 1) for i in range(step - 1, size - 1)])
        right = lax.ppermute(right, "sp", [(i, i - 1) for i in range(1, size - step + 1)])
        from_left[step] = [left] + swap_parts(left, range(step, size))
        from_right[step] = [right] + swap_parts(right, range(size - step))
    for j in range(1, size):
        chunks.append(
            [
                jnp.where(mine + j < size, after, before)
                for after, before in zip(from_right[j], from_left[size - j])
            ]
        )
    return chunks, [(from_left[k][0], from_right[k][0]) for k in range(1, size)]


def scatter_sum(x):
    size, member = lax.axis_size("tp"), lax.axis_index("tp")
    if size & (size - 1):
        return lax.psum_scatter(x, "tp", scatter_dimension=0, tiled=True).astype(jnp.float32)
    rest, width = size, x.shape[1]
    portion = x.shape[0] // size
    bit = 1
    total = x
    while bit < size:
        rest //= 2
        here = (member // bit) % 2
        split = total.reshape(rest, 2, portion, width)
        keep = lax.dynamic_index_in_dim(split, here, 1, keepdims=False)
        send = lax.dynamic_index_in_dim(split, 1 - here, 1, keepdims=False).astype(jnp.bfloat16)
        got = lax.ppermute(send, "tp", [(i, i ^ bit) for i in range(size)])
        total = keep.astype(jnp.float32) + got.astype(jnp.float32)
        bit *= 2
    return total.reshape(portion, width)


def gather_rows(x):
    size, member = lax.axis_size("tp"), lax.axis_index("tp")
    if size & (size - 1):
        return lax.all_gather(x, "tp", axis=0, tiled=True)
    portion, width = x.shape
    whole = x[None]
    bit = size // 2
    while bit:
        here = (member // bit) % 2
        got = lax.ppermute(whole, "tp", [(i, i ^ bit) for i in range(size)])
        first = jnp.where(here == 0, whole, got)
        second = jnp.where(here == 0, got, whole)
        whole = jnp.stack([first, second], axis=1).reshape(-1, portion, width)
        bit //= 2
    return whole.reshape(size * portion, width)


def retain_local(queries, key_rows, value_rows, log_decay):
    total_heads = log_decay.shape[0]
    length = queries.shape[0]
    key_width = queries.shape[1] // total_heads
    value_width = value_rows.shape[1] // total_heads
    query_heads = queries.reshape(length, total_heads, key_width)
    key_heads = key_rows.reshape(length, total_heads, key_width)
    value_heads = value_rows.reshape(length, total_heads, value_width)
    cumulative = jnp.cumsum(log_decay, axis=1)
    row_index = lax.broadcasted_iota(jnp.int32, (length, length), 0)
    col_index = lax.broadcasted_iota(jnp.int32, (length, length), 1)
    causal = (row_index >= col_index)[None]
    log_gap = cumulative[:, :, None] - cumulative[:, None, :]
    fading = jnp.where(causal, jnp.exp(jnp.where(causal, log_gap, 0.0)), 0.0)
    scores = jnp.einsum("ihd,jhd->hij", query_heads, key_heads, preferred_element_type=jnp.float32)
    weights_low = (scores * key_width ** (-0.5) * fading).astype(jnp.bfloat16)
    within = jnp.einsum(
        "hij,jhe->ihe", weights_low, value_heads, preferred_element_type=jnp.float32
    )
    to_end = jnp.exp(cumulative[:, -1:] - cumulative)
    keyed = (key_heads.astype(jnp.float32) * key_width ** (-0.5) * to_end.T[:, :, None]).astype(
        jnp.bfloat16
    )
    local_state = jnp.einsum("jhd,jhe->hde", keyed, value_heads, preferred_element_type=jnp.float32)
    return (query_heads, cumulative, within, cumulative[:, -1], local_state)


def finish(query_heads, cumulative, within, incoming, gain_values):
    carried = (
        jnp.einsum(
            "ihd,hde->ihe",
            query_heads,
            incoming.astype(jnp.bfloat16),
            preferred_element_type=jnp.float32,
        )
        * jnp.exp(cumulative).T[:, :, None]
    )
    retained = within + carried
    centered = retained - jnp.mean(retained, axis=-1, keepdims=True)
    scaled = centered * lax.rsqrt(jnp.mean(centered * centered, axis=-1, keepdims=True) + EPS)
    return (scaled.reshape(retained.shape[0], -1) * gain_values).astype(jnp.bfloat16)


def normalize(rows, gain_values):
    values = rows.astype(jnp.float32)
    scaled = values * lax.rsqrt(jnp.mean(values * values, axis=-1, keepdims=True) + EPS)
    return (scaled * gain_values).astype(jnp.bfloat16)


def on_device(
    stream_in,
    query_wide,
    key_wide,
    value_wide,
    query_narrow,
    key_narrow,
    value_narrow,
    decay_wide,
    decay_narrow,
    gain_wide,
    gain_narrow,
    out_wide,
    out_narrow,
    mlp_gain,
    up_weight,
    down_weight,
):
    length = stream_in.shape[0]
    portion = length // lax.axis_size("tp")
    member = lax.axis_index("tp")
    up_chunks, up_steps = weight_chunks(up_weight, 0)
    down_chunks, down_steps = weight_chunks(down_weight, 1)
    wide_query, wide_cum, wide_within, wide_log, wide_state = retain_local(
        query_wide, key_wide, value_wide, decay_wide
    )
    thin_query, thin_cum, thin_within, thin_log, thin_state = retain_local(
        query_narrow, key_narrow, value_narrow, decay_narrow
    )
    wide_incoming, thin_incoming = incoming_state(
        (wide_state, thin_state), (wide_log, thin_log), "sp"
    )
    normed_wide = finish(wide_query, wide_cum, wide_within, wide_incoming, gain_wide)
    normed_thin = finish(thin_query, thin_cum, thin_within, thin_incoming, gain_narrow)
    normed_wide, normed_thin, _ = lax.optimization_barrier(
        (normed_wide, normed_thin, up_steps[:1])
    )
    mixed = scatter_sum(
        (
            jnp.dot(normed_wide, out_wide, preferred_element_type=jnp.float32)
            + jnp.dot(normed_thin, out_narrow, preferred_element_type=jnp.float32)
        ).astype(jnp.bfloat16)
    )
    stream_rows = lax.dynamic_slice_in_dim(stream_in, member * portion, portion, 0)
    middle = (stream_rows.astype(jnp.float32) + mixed).astype(jnp.bfloat16)
    middle, _ = lax.optimization_barrier((middle, (down_steps[:1], up_steps[1:2])))
    normed = gather_rows(normalize(middle, mlp_gain))
    groups, size = lax.axis_size("grp"), lax.axis_size("sp")
    group, mine = lax.axis_index("grp"), lax.axis_index("sp")
    depth = up_weight.shape[0]
    turned = jnp.roll(normed, -mine * depth, axis=1)
    turned = turned.reshape(length, size, groups, depth // groups)
    turned = jnp.roll(turned, -group, axis=2).reshape(length, -1)
    up_full = jnp.concatenate([part for chunk in up_chunks for part in chunk], axis=0)
    raised = jax.nn.relu(jnp.dot(turned, up_full, preferred_element_type=jnp.float32))
    hidden = (raised * raised).astype(jnp.bfloat16)
    blocks = []
    for chunk in down_chunks:
        partial = jnp.concatenate(
            [jnp.dot(hidden, part, preferred_element_type=jnp.float32) for part in chunk], axis=1
        )
        blocks.append(scatter_sum(partial.astype(jnp.bfloat16)))
    channel = jnp.stack(blocks, axis=1).reshape(portion, size, groups, -1)
    channel = jnp.roll(channel, group, axis=2).reshape(portion, -1)
    channel = jnp.roll(channel, mine * down_weight.shape[1], axis=1)
    return (middle.astype(jnp.float32) + channel).astype(jnp.bfloat16)


def solution(mesh):
    placed = (
        P(("grp", "sp"), None),
        P(("grp", "sp"), "tp"),
        P(("grp", "sp"), "tp"),
        P(("grp", "sp"), "tp"),
        P(("grp", "sp"), "tp"),
        P(("grp", "sp"), "tp"),
        P(("grp", "sp"), "tp"),
        P("tp", ("grp", "sp")),
        P("tp", ("grp", "sp")),
        P("tp"),
        P("tp"),
        P("tp", None),
        P("tp", None),
        P(),
        P("sp", "tp"),
        P("tp", "sp"),
    )
    return jax.shard_map(
        on_device,
        mesh=mesh,
        in_specs=placed,
        out_specs=P(("grp", "sp", "tp"), None),
        check_vma=False,
    )
```
